32 devices in a mesh: fs: 4 (over z), rep: 2 (over y), tp: 4 (over x, core).
Axes of the slice: x: 2, y: 2, z: 4, core: 2. Of those that a mesh axis runs over, the one named last changes fastest.
Arguments:
- saved_hidden: bfloat16 [7168, 2048], P(('fs', 'rep')), may hold values from -12 to 12
- grad_value: bfloat16 [7168, 1024], P(('fs', 'rep'), 'tp'), may hold values from -12 to 12
- saved_mixed: bfloat16 [7168, 1024], P(('fs', 'rep'), 'tp'), may hold values from -12 to 12
- grad_output: bfloat16 [7168, 2048], P(('fs', 'rep')), may hold values from -12 to 12
- basis_value: bfloat16 [2048, 128], replicated, may hold values from -0.5 to 0.5
- basis_output: bfloat16 [2048, 128], replicated, may hold values from -0.5 to 0.5
- weight_value: float32 [2048, 1024], P('fs', 'tp'), may hold values from -0.125 to 0.125
- weight_output: float32 [1024, 2048], P('tp', 'fs'), may hold values from -0.1875 to 0.1875
- first_value: float32 [128, 1024], P('fs', 'tp'), may hold values from -4 to 4
- second_value: float32 [128, 1024], P('fs', 'tp'), may hold values from 0.05 to 0.5
- first_output: float32 [128, 1024], P('fs', 'tp'), may hold values from -4 to 4
- second_output: float32 [128, 1024], P('fs', 'tp'), may hold values from 0.05 to 0.5
Outputs:
- step_value: float32 [2048, 1024], P('fs', 'tp')
- step_output: float32 [1024, 2048], P('tp', 'fs')
- new_weight_value: float32 [2048, 1024], P('fs', 'tp')
- new_weight_output: float32 [1024, 2048], P('tp', 'fs')
- copy_value: bfloat16 [2048, 1024], P(None, 'tp')
- copy_output: bfloat16 [1024, 2048], P('tp')
- new_first_value: float32 [128, 1024], P('fs', 'tp')
- new_second_value: float32 [128, 1024], P('fs', 'tp')
- new_first_output: float32 [128, 1024], P('fs', 'tp')
- new_second_output: float32 [128, 1024], P('fs', 'tp')
The draws below stay inside these ranges and needn't reach their ends.
All inputs are finite; a program needn't handle non-finite values.
Results may differ from the reference program's by a relative error of at most 0.0045.
Values may be sent and summed in bfloat16 or wider, within the bound.
No kernel may reach another device: no remote copies, remote signals or barrier semaphores. Data moves between devices by JAX's collectives and lax.ppermute only.
A program may use at most 64 MiB of HBM per device.

```python
import math
import jax
import jax.numpy as jnp
from jax import lax

D = 2048
AW = 1024
RANK = 128
TOKENS = 7168


def field_values(key, row_total, col_total, rising_columns):
    key_noise = jax.random.fold_in(key, 0)
    length = col_total if rising_columns else row_total
    position = jnp.arange(length, dtype=jnp.float32) / max(length - 1, 1)
    noise_field = jnp.clip(jax.random.normal(key_noise, (row_total, col_total), jnp.float32), -4.0, 4.0)
    scales = jnp.exp(math.log(3.0) * position)
    if rising_columns:
        return noise_field * scales[None, :]
    return noise_field * scales[:, None]


def draw_saved_hidden(key, part):
    return field_values(jax.random.fold_in(key, 11), TOKENS, D, False).astype(jnp.bfloat16)


def draw_grad_value(key, part):
    return field_values(jax.random.fold_in(key, 23), TOKENS, AW, True).astype(jnp.bfloat16)


def draw_saved_mixed(key, part):
    return field_values(jax.random.fold_in(key, 37), TOKENS, AW, True).astype(jnp.bfloat16)


def draw_grad_output(key, part):
    return field_values(jax.random.fold_in(key, 41), TOKENS, D, False).astype(jnp.bfloat16)


def steps_of(own_key, extent, cuts, smallest, top_value):
    loudness = 1.0
    for axis_at, shards_of in cuts:
        heights = jax.random.uniform(jax.random.fold_in(jax.random.fold_in(own_key, 6), axis_at), (shards_of,), jnp.float32, smallest / len(cuts), top_value / len(cuts))
        loudness = loudness * jnp.repeat(jnp.exp(heights), extent[axis_at] // shards_of).reshape((-1,) + (1,) * (len(extent) - 1 - axis_at))
    return loudness


def centred(rng, dims, scale, most, cuts=(), held_as=jnp.bfloat16):
    result = scale * jax.random.normal(rng, dims, jnp.float32)
    if cuts:
        result = result * steps_of(rng, dims, cuts, -0.22, 0.18)
    return jnp.clip(result, -most, most).astype(held_as)


def setup_inputs(seed: int = 0) -> dict:
    streams_of = jax.random.split(jax.random.key(seed), 13)
    return {
        "saved_hidden": draw_saved_hidden(jax.random.fold_in(streams_of[12], 71), 0),
        "grad_value": draw_grad_value(jax.random.fold_in(streams_of[12], 71), 0),
        "saved_mixed": draw_saved_mixed(jax.random.fold_in(streams_of[12], 71), 0),
        "grad_output": draw_grad_output(jax.random.fold_in(streams_of[12], 71), 0),
        "basis_value": centred(streams_of[4], (D, RANK), RANK ** -0.5, 0.5),
        "basis_output": centred(streams_of[5], (D, RANK), RANK ** -0.5, 0.5),
        "weight_value": centred(streams_of[6], (D, AW), D ** -0.5, 0.125, ((0, 4), (1, 4)), jnp.float32),
        "weight_output": centred(streams_of[7], (AW, D), AW ** -0.5, 0.1875, ((0, 4), (1, 4)), jnp.float32),
        "first_value": centred(streams_of[8], (RANK, AW), 1.0, 4.0, ((0, 4), (1, 4)), jnp.float32),
        "second_value": jnp.clip(jnp.exp(math.log(0.5) - 2.3025851 * jax.random.uniform(streams_of[9], (RANK, AW), jnp.float32) ** steps_of(streams_of[9], (RANK, AW), ((0, 4), (1, 4)), -0.2, 0.2)), 0.05, 0.5),
        "first_output": centred(streams_of[10], (RANK, AW), 1.0, 4.0, ((0, 4), (1, 4)), jnp.float32),
        "second_output": jnp.clip(jnp.exp(math.log(0.5) - 2.3025851 * jax.random.uniform(streams_of[11], (RANK, AW), jnp.float32) ** steps_of(streams_of[11], (RANK, AW), ((0, 4), (1, 4)), -0.2, 0.2)), 0.05, 0.5),
    }


first_decay = 0.8
second_decay = 0.9
learning_rate = 0.02
norm_epsilon = 1e-06

def project(basis, gradient):
    return jnp.dot(basis.astype(jnp.float32).T, gradient, precision=lax.Precision.HIGHEST)

def moments(projected, first_old, second_old, clip_factor):
    scaled = clip_factor * projected
    first_new = first_decay * first_old + (1.0 - first_decay) * scaled
    second_new = second_decay * second_old + (1.0 - second_decay) * scaled * scaled
    return (first_new, second_new, first_new / jnp.sqrt(second_new))

def reference(saved_hidden, grad_value, saved_mixed, grad_output, basis_value, basis_output, weight_value, weight_output, first_value, second_value, first_output, second_output):
    gradient_value = jnp.dot(saved_hidden.T, grad_value, preferred_element_type=jnp.float32)
    gradient_output = jnp.dot(grad_output.T, saved_mixed, preferred_element_type=jnp.float32)
    projected_value = project(basis_value, gradient_value)
    projected_output = project(basis_output, gradient_output)
    squares = jnp.sum(projected_value * projected_value) + jnp.sum(projected_output * projected_output)
    mean_square = squares / (2 * RANK * AW)
    clip_factor = jnp.minimum(1.0, 1.0 / jnp.sqrt(mean_square + norm_epsilon))
    first_new_value, second_new_value, direction_value = moments(projected_value, first_value, second_value, clip_factor)
    first_new_output, second_new_output, direction_output = moments(projected_output, first_output, second_output, clip_factor)
    step_value = jnp.dot(basis_value.astype(jnp.float32), direction_value, precision=lax.Precision.HIGHEST)
    step_output = jnp.dot(basis_output.astype(jnp.float32), direction_output, precision=lax.Precision.HIGHEST).T
    new_weight_value = weight_value - learning_rate * step_value
    new_weight_output = weight_output - learning_rate * step_output
    return (step_value, step_output, new_weight_value, new_weight_output, new_weight_value.astype(jnp.bfloat16), new_weight_output.astype(jnp.bfloat16), first_new_value, second_new_value, first_new_output, second_new_output)
```

```python
import jax
import jax.numpy as jnp
from jax import lax
from jax.experimental import pallas as pl
from jax.experimental.pallas import tpu as pltpu
from jax.sharding import PartitionSpec as P


first_decay = 0.8
second_decay = 0.9
learning_rate = 0.02
norm_epsilon = 1e-06
contract_leading = (((0,), (0,)), ((), ()))
contract_trailing = (((1,), (1,)), ((), ()))
f32 = jnp.float32
bf16 = jnp.bfloat16


def moments(projected, first_old, second_old, clip_factor):
    scaled = clip_factor * projected
    first_new = first_decay * first_old + (1.0 - first_decay) * scaled
    second_new = second_decay * second_old + (1.0 - second_decay) * scaled * scaled
    return (first_new, second_new, first_new / jnp.sqrt(second_new))


def on_chip(array):
    return pltpu.with_memory_space_constraint(array, pltpu.VMEM)


def exchange(array, axis, size, distance):
    return lax.ppermute(array, axis, [(i, i ^ distance) for i in range(size)])


def limit(mib):
    return pltpu.CompilerParams(vmem_limit_bytes=mib << 20)


VM = pl.BlockSpec(memory_space=pltpu.VMEM)
ANY = pl.BlockSpec(memory_space=pl.ANY)


def split_halves(value):
    upper = value.astype(bf16)
    lower = (value - upper.astype(f32)).astype(bf16)
    return upper, lower


def partial_product(rows, basis, other):
    reduced = jnp.dot(rows, basis, preferred_element_type=f32)
    rank = reduced.shape[1]
    upper, lower = split_halves(reduced)
    stacked = jnp.concatenate([upper, lower], axis=1)
    both = lax.dot_general(stacked, other, contract_leading, preferred_element_type=f32)
    return both[:rank] + both[rank:]


def value_kernel(rows, basis, other, out):
    out[...] = partial_product(rows[...], basis[...], other[...])


def output_kernel(rows, basis, other, value_part, keep, send):
    part = partial_product(rows[...], basis[...], other[...])
    mine = lax.axis_index("rep")

    @pl.when(mine == 0)
    def _():
        keep[...] = value_part[...]
        send[...] = part.astype(send.dtype)

    @pl.when(mine != 0)
    def _():
        keep[...] = part
        send[...] = value_part[...].astype(send.dtype)


def square_kernel(mine, other, message, squares):
    rank = mine.shape[0]
    total = mine[...].astype(f32) + other[...].astype(f32)
    message[pl.ds(0, rank), :] = total
    tile = jnp.broadcast_to(jnp.sum(total * total), squares.shape)
    squares[...] = tile
    message[pl.ds(rank, 8), :] = jnp.broadcast_to(tile[0:1, 0:1], (8, total.shape[1]))


def final_kernel(
    count,
    basis_rows,
    own,
    got,
    squares,
    squares_other,
    firsts_value,
    seconds_value,
    firsts_output,
    seconds_output,
    weight_value,
    weight_output,
    basis_value,
    basis_output,
    z1,
    z2,
    z3,
    y1,
    y2,
    y3,
    step_value,
    step_output,
    new_weight_value,
    new_weight_output,
    copy_value,
    copy_output,
    new_first_value,
    new_second_value,
    new_first_output,
    new_second_output,
    projected,
    firsts,
    seconds,
    step_v,
    step_o,
    new_v,
    new_o,
    block_v,
    block_o,
    nfv,
    nsv,
    nfo,
    nso,
    sems,
):
    fs_index = lax.axis_index("fs")
    rep_index = lax.axis_index("rep")
    rank = basis_value.shape[1]
    part_rows = firsts_value.shape[0]
    rows = weight_value.shape[0]
    half = rows // 2
    width = weight_value.shape[1]
    copies = []

    def send(source, target):
        copy = pltpu.make_async_copy(source, target, sems.at[len(copies)])
        copy.start()
        copies.append(copy)

    projected[rep_index] = own[pl.ds(0, rank), :]
    projected[1 - rep_index] = got[pl.ds(0, rank), :]
    mean_square = (squares[...] + squares_other[...])[0:1, 0:1] / count
    clip_factor = jnp.minimum(1.0, 1.0 / jnp.sqrt(mean_square + norm_epsilon))

    is_end = jnp.logical_or(fs_index == 0, fs_index == 3)
    sources = (
        fs_index ^ 1,
        jnp.where(is_end, fs_index ^ 2, fs_index ^ 3),
        jnp.where(is_end, fs_index ^ 3, fs_index ^ 2),
    )
    own_at = pl.multiple_of(fs_index * part_rows, part_rows)
    held = ((firsts_value, seconds_value, nfv, nsv), (firsts_output, seconds_output, nfo, nso))
    targets = ((new_first_value, new_second_value), (new_first_output, new_second_output))
    for m in range(2):
        first_old, second_old, nf, ns = held[m]
        firsts[m, pl.ds(own_at, part_rows), :] = first_old[...].astype(bf16).astype(f32)
        seconds[m, pl.ds(own_at, part_rows), :] = second_old[...].astype(bf16).astype(f32)
        new_first, new_second, _ = moments(
            projected[m, pl.ds(own_at, part_rows), :], first_old[...], second_old[...], clip_factor
        )
        nf[...] = new_first
        ns[...] = new_second
        send(nf, targets[m][0])
        send(ns, targets[m][1])
    for source, z, y in zip(sources, (z1, z2, z3), (y1, y2, y3)):
        at = pl.multiple_of(source * part_rows, part_rows)
        for m, ref in ((rep_index, z), (1 - rep_index, y)):
            firsts[m, pl.ds(at, part_rows), :] = ref[pl.ds(2 * half, part_rows), :].astype(f32)
            seconds[m, pl.ds(at, part_rows), :] = ref[
                pl.ds(2 * half + part_rows, part_rows), :
            ].astype(f32)

    stacked = []
    for m in range(2):
        _, _, direction = moments(projected[m], firsts[m], seconds[m], clip_factor)
        if m == 1:
            direction = direction.T
        upper, lower = split_halves(direction)
        stacked.append(jnp.concatenate([upper, lower], axis=m))

    def steps_of(first_row, row_count):
        at = pl.multiple_of(first_row, row_count)
        b = basis_value[pl.ds(at, row_count), :]
        sv = jnp.dot(jnp.concatenate([b, b], axis=1), stacked[0], preferred_element_type=f32)
        b = basis_output[pl.ds(at, row_count), :]
        so = lax.dot_general(
            stacked[1],
            jnp.concatenate([b, b], axis=1),
            contract_trailing,
            preferred_element_type=f32,
        )
        return sv, so

    sv, so = steps_of(fs_index * rows, rows)
    step_v[...] = sv
    send(step_v, step_value)
    step_o[...] = so
    send(step_o, step_output)
    new_v[...] = weight_value[...] - learning_rate * sv
    send(new_v, new_weight_value)
    new_o[...] = weight_output[...] - learning_rate * so
    send(new_o, new_weight_output)
    at = pl.multiple_of(fs_index * rows, rows)
    for slot in range(4):
        if slot == 0:
            source = fs_index
            blocks = [(0, None), (1, None)]
        else:
            source = sources[slot - 1]
            blocks = [(rep_index, (z1, z2, z3)[slot - 1]), (1 - rep_index, (y1, y2, y3)[slot - 1])]
        for j, (h, ref) in enumerate(blocks):
            first_row = source * rows + h * half
            at = pl.multiple_of(first_row, half)
            if ref is None:
                sv = step_v[pl.ds(h * half, half), :]
                so = step_o[:, pl.ds(h * half, half)]
                wv = weight_value[pl.ds(h * half, half), :].astype(bf16).astype(f32)
                wo = weight_output[:, pl.ds(h * half, half)].astype(bf16).astype(f32)
            else:
                sv, so = steps_of(first_row, half)
                wv = ref[pl.ds(0, half), :].astype(f32)
                wo = ref[pl.ds(half, half), :].astype(f32)
            n = 2 * slot + j
            block_v[n] = (wv - learning_rate * sv).astype(bf16)
            send(block_v.at[n], copy_value.at[pl.ds(at, half), :])
            block_o[n] = (wo - learning_rate * so).astype(bf16)
            send(block_o.at[n], copy_output.at[:, pl.ds(at, half)])
    for copy in copies:
        copy.wait()


def paired(
    saved_hidden,
    grad_value,
    saved_mixed,
    grad_output,
    basis_value,
    basis_output,
    weight_value,
    weight_output,
    first_value,
    second_value,
    first_output,
    second_output,
    sizes,
):
    fs, rep, tp = sizes
    rows, width = weight_value.shape
    half = rows // 2
    rank = basis_value.shape[1]
    part_rows = first_value.shape[0]
    model = basis_value.shape[0]
    fs_index = lax.axis_index("fs")
    rep_index = lax.axis_index("rep")

    held = jnp.concatenate([first_value, second_value, first_output, second_output], axis=0)
    packed = jnp.concatenate(
        [
            lax.dynamic_slice_in_dim(weight_value, rep_index * half, half, 0),
            lax.dynamic_slice_in_dim(weight_output, rep_index * half, half, 1),
            lax.dynamic_slice_in_dim(held, rep_index * 2 * part_rows, 2 * part_rows, 0),
        ],
        axis=0,
    ).astype(bf16)
    ends = [(1, 0), (2, 3)]
    middles = [(1, 2), (2, 1)]
    is_end = jnp.logical_or(fs_index == 0, fs_index == fs - 1)
    z1 = exchange(packed, "fs", fs, 1)
    m1 = lax.ppermute(packed, "fs", middles)
    m2 = lax.ppermute(z1, "fs", middles)
    x2 = lax.ppermute(m1, "fs", ends)
    x3 = lax.ppermute(m2, "fs", ends)
    z2 = jnp.where(is_end, x2, m1)
    z3 = jnp.where(is_end, x3, m2)
    y1 = exchange(z1, "rep", rep, 1)
    y2 = exchange(z2, "rep", rep, 1)
    y3 = exchange(z3, "rep", rep, 1)

    shape = (rank, width)
    value_part = pl.pallas_call(
        value_kernel,
        out_shape=pltpu.VMEM(shape, f32),
        in_specs=[VM] * 3,
        out_specs=VM,
        compiler_params=limit(12),
        name="value_part",
    )(on_chip(saved_hidden), on_chip(basis_value), on_chip(grad_value))
    keep, send = pl.pallas_call(
        output_kernel,
        out_shape=(pltpu.VMEM(shape, f32), pltpu.VMEM(shape, bf16)),
        in_specs=[VM] * 4,
        out_specs=(VM, VM),
        compiler_params=limit(12),
        name="output_part",
    )(on_chip(grad_output), on_chip(basis_output), on_chip(saved_mixed), value_part)
    total = keep + exchange(send, "rep", rep, 1).astype(f32)
    for distance in (1,):
        rounded = total.astype(bf16)
        total = rounded.astype(f32) + exchange(rounded, "fs", fs, distance).astype(f32)
    rounded = total.astype(bf16)
    message, squares = pl.pallas_call(
        square_kernel,
        out_shape=(pltpu.VMEM((rank + 8, width), f32), pltpu.VMEM((8, 128), f32)),
        in_specs=[VM] * 2,
        out_specs=(VM, VM),
        compiler_params=limit(4),
        name="squares",
    )(on_chip(rounded), on_chip(exchange(rounded, "fs", fs, 2)))
    got = exchange(message, "rep", rep, 1)
    across = exchange(squares, "tp", tp, 2)
    diagonal = lax.ppermute(
        squares,
        ("rep", "tp"),
        [(i * tp + j, (i ^ 1) * tp + (j ^ 2)) for i in range(rep) for j in range(tp)],
    )
    four = (squares + got[rank:, :128]) + (across + diagonal)
    four_other = exchange(four, "tp", tp, 1)

    outs = (
        jax.ShapeDtypeStruct((rows, width), f32),
        jax.ShapeDtypeStruct((width, rows), f32),
        jax.ShapeDtypeStruct((rows, width), f32),
        jax.ShapeDtypeStruct((width, rows), f32),
        jax.ShapeDtypeStruct((model, width), bf16),
        jax.ShapeDtypeStruct((width, model), bf16),
    ) + tuple(jax.ShapeDtypeStruct((part_rows, width), f32) for _ in range(4))
    scratch = (
        [pltpu.VMEM((2, rank, width), f32)] * 3
        + [pltpu.VMEM((rows, width), f32), pltpu.VMEM((width, rows), f32)] * 2
        + [pltpu.VMEM((2 * fs, half, width), bf16), pltpu.VMEM((2 * fs, width, half), bf16)]
        + [pltpu.VMEM((part_rows, width), f32)] * 4
        + [pltpu.SemaphoreType.DMA((8 + 4 * fs,))]
    )

    def kernel(*refs):
        final_kernel(2 * rank * width * tp, rows, *refs)

    operands = (
        message,
        got,
        four,
        four_other,
        first_value,
        second_value,
        first_output,
        second_output,
        weight_value,
        weight_output,
        basis_value,
        basis_output,
        z1,
        z2,
        z3,
        y1,
        y2,
        y3,
    )
    return pl.pallas_call(
        kernel,
        out_shape=outs,
        in_specs=[VM] * len(operands),
        out_specs=(ANY,) * len(outs),
        scratch_shapes=scratch,
        compiler_params=limit(24),
        name="finish",
    )(*[on_chip(operand) for operand in operands])


def plain(
    saved_hidden,
    grad_value,
    saved_mixed,
    grad_output,
    basis_value,
    basis_output,
    weight_value,
    weight_output,
    first_value,
    second_value,
    first_output,
    second_output,
    sizes,
):
    row_count, width = weight_value.shape
    moment_count = first_value.shape[0]
    rank = basis_value.shape[1]
    fs_index = lax.axis_index("fs")
    row_first = fs_index * row_count
    moment_first = fs_index * moment_count
    value_basis_rows = lax.dynamic_slice_in_dim(basis_value, row_first, row_count, 0).astype(f32)
    output_basis_rows = lax.dynamic_slice_in_dim(basis_output, row_first, row_count, 0).astype(f32)
    part_value = partial_product(saved_hidden, basis_value, grad_value)
    part_output = partial_product(grad_output, basis_output, saved_mixed)
    projected_value, projected_output = lax.psum((part_value, part_output), ("fs", "rep"))
    local_squares = jnp.sum(projected_value * projected_value) + jnp.sum(
        projected_output * projected_output
    )
    total_squares = lax.psum(local_squares, "tp")
    mean_square = total_squares / (2 * rank * width * sizes[2])
    clip_factor = jnp.minimum(1.0, 1.0 / jnp.sqrt(mean_square + norm_epsilon))
    value_slice = lax.dynamic_slice_in_dim(projected_value, moment_first, moment_count, 0)
    output_slice = lax.dynamic_slice_in_dim(projected_output, moment_first, moment_count, 0)
    new_first_value, new_second_value, value_direction_rows = moments(
        value_slice, first_value, second_value, clip_factor
    )
    new_first_output, new_second_output, output_direction_rows = moments(
        output_slice, first_output, second_output, clip_factor
    )
    direction_value = lax.all_gather(value_direction_rows, "fs", axis=0, tiled=True)
    direction_output = lax.all_gather(output_direction_rows, "fs", axis=0, tiled=True)
    step_value = jnp.dot(value_basis_rows, direction_value, precision=lax.Precision.HIGHEST)
    step_output = jnp.dot(output_basis_rows, direction_output, precision=lax.Precision.HIGHEST).T
    new_weight_value = weight_value - learning_rate * step_value
    new_weight_output = weight_output - learning_rate * step_output
    copy_value = lax.all_gather(new_weight_value.astype(bf16), "fs", axis=0, tiled=True)
    copy_output = lax.all_gather(new_weight_output.astype(bf16), "fs", axis=1, tiled=True)
    return (
        step_value,
        step_output,
        new_weight_value,
        new_weight_output,
        copy_value,
        copy_output,
        new_first_value,
        new_second_value,
        new_first_output,
        new_second_output,
    )


def solution(mesh):
    sizes = tuple(mesh.shape[axis] for axis in ("fs", "rep", "tp"))
    chosen = paired if sizes == (4, 2, 4) else plain

    def local(*args):
        return chosen(*args, sizes)

    return jax.shard_map(
        local,
        mesh=mesh,
        in_specs=(
            P(("fs", "rep"), None),
            P(("fs", "rep"), "tp"),
            P(("fs", "rep"), "tp"),
            P(("fs", "rep"), None),
            P(),
            P(),
            P("fs", "tp"),
            P("tp", "fs"),
            P("fs", "tp"),
            P("fs", "tp"),
            P("fs", "tp"),
            P("fs", "tp"),
        ),
        out_specs=(
            P("fs", "tp"),
            P("tp", "fs"),
            P("fs", "tp"),
            P("tp", "fs"),
            P(None, "tp"),
            P("tp", None),
            P("fs", "tp"),
            P("fs", "tp"),
            P("fs", "tp"),
            P("fs", "tp"),
        ),
        check_vma=False,
    )
```
